32 devices in a mesh: grp: 2 (over y), ep: 8 (over z, x), tp: 2 (over core).
Axes of the slice: x: 2, y: 2, z: 4, core: 2. Of those that a mesh axis runs over, the one named last changes fastest.
Arguments:
- tokens: bfloat16 [4096, 2048], P(('grp', 'ep'), 'tp'), parts along dimension 0, may hold values from -6 to 6
- norm_gain: bfloat16 [2048], P('tp'), may hold values from 0.099609375 to 1.8984375
- w_gate: bfloat16 [8, 2048, 1024], P('ep', None, 'tp'), may hold values from -0.125 to 0.125
- w_up: bfloat16 [8, 2048, 1024], P('ep', None, 'tp'), may hold values from -0.125 to 0.125
- w_down: bfloat16 [8, 1024, 2048], P('ep', 'tp'), may hold values from -0.1875 to 0.1875
- expert_ids: int32 [4096, 2], P(('grp', 'ep')), parts along dimension 0, may hold values from 0 to 7, as said below
- combine: float32 [4096, 2], P(('grp', 'ep')), parts along dimension 0, may hold values from 0.1 to 1
- final_gain: bfloat16 [2048], P('tp'), may hold values from 0.099609375 to 1.8984375
Outputs:
- result: bfloat16 [4096, 2048], P(('grp', 'ep'), 'tp'), parts along dimension 0
The draws below stay inside these ranges and needn't reach their ends.
There are 2 independent parts, one for each index of `grp`. The reference program is written for one: setup_inputs(seed, part) draws one part's arguments, and reference() takes and returns one part's arrays. A program takes and returns all parts, laid end to end along the dimension named above; an argument that names none is the same for every part. Nothing has to cross between parts.
Inputs may be any that keep to these rules, and one draw needn't show every extreme that they name: `expert_ids`: the experts form 4 groups of consecutive ids of equal size; the 2 experts of a row are different and lie in one group. Among the rows of one index of ep no expert is named more than 160 times, and in each such block some expert is named exactly 160 times.
All inputs are finite; a program needn't handle non-finite values.
Results may differ from the reference program's by a relative error of at most 0.0077.
Values may be sent and summed in bfloat16 or wider, within the bound.
A program may use at most 64 MiB of HBM per device.

```python
import math
import jax
import jax.numpy as jnp
from jax import lax

D = 2048
FF = 1024
GROUPS = 4
TOP = 2
TOK_DEV = 256
EXPERTS = 8
CAP = 160
TOKENS = 2048
N_EP = 8
N_TP = 2


def draw_expert_ids(key, part):
    per_group = EXPERTS // GROUPS
    base = TOK_DEV // 8

    def one_block(block_key):
        key_busy, key_order, key_shift = jax.random.split(block_key, 3)
        busy = jax.random.randint(key_busy, (), 0, GROUPS)
        labels = jnp.arange(GROUPS, dtype=jnp.int32)
        counts = jnp.where(labels == busy, 5 * base, base).astype(jnp.int32)
        starts = jnp.cumsum(counts) - counts
        order = jax.random.permutation(key_order, TOK_DEV)
        ranks = jnp.arange(TOK_DEV, dtype=jnp.int32)
        group = jnp.sum((ranks[:, None] >= (starts + counts)[None, :]).astype(jnp.int32), axis=1)
        inner = ranks - starts[group]
        shifts = jax.random.randint(key_shift, (GROUPS,), 0, per_group)[group]
        first = (inner + shifts) % per_group
        second = (first + 1 + inner // per_group % max(per_group - 1, 1)) % per_group
        paired = jnp.stack([group * per_group + first, group * per_group + second], axis=1).astype(jnp.int32)
        return jnp.zeros((TOK_DEV, 2), jnp.int32).at[order].set(paired)
    blocks = jax.vmap(one_block)(jax.random.split(jax.random.fold_in(key, 11), TOKENS // TOK_DEV))
    return blocks.reshape(TOKENS, 2)


def block_scale(key, dims, cuts, low, high):
    loudness, own = 1.0, jax.random.fold_in(key, 6)
    for dim, blocks in cuts:
        steps = jnp.exp(jax.random.uniform(jax.random.fold_in(own, dim), (blocks,), jnp.float32, low / len(cuts), high / len(cuts)))
        loudness = loudness * jnp.repeat(steps, dims[dim] // blocks).reshape([-1 if axis == dim else 1 for axis in range(len(dims))])
    return loudness


def scatter_about(rng, dims, deviation, reach, cuts=(), held_as=jnp.bfloat16):
    array = deviation * jax.random.normal(rng, dims, jnp.float32)
    if cuts:
        array = array * block_scale(rng, dims, cuts, -0.22, 0.18)
    return jnp.clip(array, -reach, reach).astype(held_as)


def setup_inputs(seed: int = 0, part: int = 0) -> dict:
    key_of = jax.random.split(jax.random.key(seed), 9)
    own_keys = jax.random.split(jax.random.fold_in(key_of[8], part), 9)
    tokens = scatter_about(own_keys[0], (TOKENS, D), 1.0, 6.0, ((0, 8), (1, 2)))
    norm_gain = jnp.clip(1.0 + 0.18 * jax.random.normal(key_of[1], (D,), jnp.float32), 0.099609375, 1.8984375).astype(jnp.bfloat16)
    w_gate = scatter_about(key_of[2], (EXPERTS, D, FF), D ** -0.5, 0.125, ((0, 8), (2, 2)))
    w_up = scatter_about(key_of[3], (EXPERTS, D, FF), D ** -0.5, 0.125, ((0, 8), (2, 2)))
    w_down = scatter_about(key_of[4], (EXPERTS, FF, D), FF ** -0.5, 0.1875, ((0, 8), (1, 2)))
    expert_ids = draw_expert_ids(jax.random.fold_in(jax.random.fold_in(key_of[8], part), 71), part)
    combine = jnp.clip(jnp.exp(math.log(1.0) - 2.3025851 * jax.random.uniform(own_keys[6], (TOKENS, TOP), jnp.float32) ** block_scale(own_keys[6], (TOKENS, TOP), ((0, 8),), -0.2, 0.2)), 0.1, 1.0)
    final_gain = jnp.clip(1.0 + 0.18 * jax.random.normal(key_of[7], (D,), jnp.float32), 0.099609375, 1.8984375).astype(jnp.bfloat16)
    return dict(tokens=tokens, norm_gain=norm_gain, w_gate=w_gate, w_up=w_up, w_down=w_down, expert_ids=expert_ids, combine=combine, final_gain=final_gain)


def reference(tokens, norm_gain, w_gate, w_up, w_down, expert_ids, combine, final_gain):
    eps = 1e-06
    xf = tokens.astype(jnp.float32)
    normed = (xf * lax.rsqrt(lax.optimization_barrier(jnp.mean(xf * xf, axis=-1, keepdims=True)) + eps) * norm_gain.astype(jnp.float32)).astype(jnp.bfloat16)
    flat = expert_ids.reshape(-1)
    weights = combine.reshape(-1)
    limit = N_EP * CAP
    half_ff = FF // N_TP

    def step(acc, expert):
        hits = flat == expert
        pos = jnp.nonzero(hits, size=limit, fill_value=0)[0].astype(jnp.int32)
        live = jnp.arange(limit, dtype=jnp.int32) < jnp.sum(hits.astype(jnp.int32))
        owner = pos // TOP
        rows = normed[owner].astype(jnp.float32)
        gate_w = lax.dynamic_index_in_dim(w_gate, expert, 0, keepdims=False).astype(jnp.float32)
        up_w = lax.dynamic_index_in_dim(w_up, expert, 0, keepdims=False).astype(jnp.float32)
        down_w = lax.dynamic_index_in_dim(w_down, expert, 0, keepdims=False).astype(jnp.float32)
        gate = jnp.dot(rows, gate_w, preferred_element_type=jnp.float32)
        upper = jnp.dot(rows, up_w, preferred_element_type=jnp.float32)
        hidden = (jax.nn.silu(gate) * upper).astype(jnp.bfloat16)
        parts = jnp.einsum('rjf,jfd->jrd', hidden.astype(jnp.float32).reshape(limit, N_TP, half_ff), down_w.reshape(N_TP, half_ff, D)).astype(jnp.bfloat16)
        parts = lax.optimization_barrier(parts)
        summed = lax.optimization_barrier(jnp.sum(parts.astype(jnp.float32), axis=0)).astype(jnp.bfloat16)
        summed = lax.optimization_barrier(summed)
        scale = jnp.where(live, weights[pos], jnp.float32(0.0))
        acc = acc.at[owner].add(scale[:, None] * summed.astype(jnp.float32))
        return (acc, None)
    mixed, _ = lax.scan(step, jnp.zeros((TOKENS, D), jnp.float32), jnp.arange(EXPERTS, dtype=jnp.int32))
    norm = lax.rsqrt(lax.optimization_barrier(jnp.mean(mixed * mixed, axis=-1, keepdims=True)) + eps)
    return (mixed * norm * final_gain.astype(jnp.float32)).astype(jnp.bfloat16)
```

```python
import functools

import jax
import jax.numpy as jnp
from jax import lax
from jax.experimental import pallas as pl
from jax.experimental.pallas import tpu as pltpu
from jax.sharding import PartitionSpec as P

GROUPS = 4
EPS = 1e-06
MESH = pl.DeviceIdType.MESH
bf16, f32 = jnp.bfloat16, jnp.float32


def general(tokens, norm_gain, w_gate, w_up, w_down, expert_ids, combine, final_gain):
    eps = EPS
    tok_dev, half = tokens.shape
    n_ep = lax.axis_size("ep")
    n_tp = lax.axis_size("tp")
    width = half * n_tp
    exp_dev = w_gate.shape[0]
    experts = exp_dev * n_ep
    per_group = experts // GROUPS
    capacity = tok_dev // 8 * 5 * 2 // per_group
    top = expert_ids.shape[1]
    narrow = tokens.astype(jnp.float32)
    squares = lax.psum(jnp.sum(narrow * narrow, axis=1), "tp")
    scale = lax.rsqrt(squares[:, None] / width + eps)
    normed = (narrow * scale * norm_gain.astype(jnp.float32)).astype(jnp.bfloat16)
    columns = normed.shape[1]
    flat = expert_ids.reshape(-1)
    onehot = (flat[:, None] == jnp.arange(experts, dtype=jnp.int32)[None, :]).astype(jnp.int32)
    ranking = jnp.sum(jnp.cumsum(onehot, axis=0) * onehot, axis=1) - 1
    target = flat * capacity + ranking
    sources = jnp.arange(tok_dev * top, dtype=jnp.int32) // top
    owner = jnp.full((experts * capacity,), tok_dev, jnp.int32).at[target].set(sources)
    padded = jnp.concatenate([normed, jnp.zeros((1, columns), jnp.bfloat16)], axis=0)
    outgoing = padded[owner].reshape(n_ep, exp_dev * capacity, columns)
    arrived = lax.all_to_all(outgoing, "ep", split_axis=0, concat_axis=0, tiled=True)
    rows = (
        arrived.reshape(n_ep, exp_dev, capacity, columns)
        .transpose(1, 0, 2, 3)
        .reshape(exp_dev, n_ep * capacity, columns)
    )
    piece = lax.all_gather(rows, "tp", axis=2, tiled=True)
    gate = jnp.einsum("erd,edf->erf", piece, w_gate, preferred_element_type=jnp.float32)
    upper = jnp.einsum("erd,edf->erf", piece, w_up, preferred_element_type=jnp.float32)
    hidden = (jax.nn.silu(gate) * upper).astype(jnp.bfloat16)
    partial_out = jnp.einsum(
        "erf,efd->erd", hidden, w_down, preferred_element_type=jnp.float32
    ).astype(jnp.bfloat16)
    shares = (
        lax.psum_scatter(partial_out, "tp", scatter_dimension=2, tiled=True)
        .astype(jnp.float32)
        .astype(jnp.bfloat16)
    )
    homeward = (
        shares.reshape(exp_dev, n_ep, capacity, half)
        .transpose(1, 0, 2, 3)
        .reshape(n_ep, exp_dev * capacity, half)
    )
    returned = lax.all_to_all(homeward, "ep", split_axis=0, concat_axis=0, tiled=True).reshape(
        experts * capacity, half
    )
    picked = returned[target].astype(jnp.float32).reshape(tok_dev, top, half)
    mixed = jnp.sum(picked * combine[:, :, None], axis=1)
    totals = lax.psum(jnp.sum(mixed * mixed, axis=1), "tp")
    norm = lax.rsqrt(totals[:, None] / width + eps)
    return (mixed * norm * final_gain.astype(jnp.float32)).astype(jnp.bfloat16)


def fold(v):
    v = v * v
    out = v[:, :128]
    for i in range(1, v.shape[1] // 128):
        out = out + v[:, i * 128 : (i + 1) * 128]
    return out


def paired_kernel(
    G, cap, tok_hbm, gain_hbm, ids_hbm, comb_hbm, fgain_hbm, wg_hbm, wu_hbm, wd_hbm, out_ref,
    wg, wu, wd, xbuf, sbuf, rawx, meta, psend, pown, precv, ebuf, xret, zbuf, ret, sq, acc,
    tok_ref, gain_ref, ids_ref, comb_ref, fgain_ref,
    fetch_s, wsem, sq_s, sq_r, z_s, z_r, m_s, m_r, x_s, x_r, t_s, t_r, p_s, p_r, e_s, e_r,
    h_s, h_r,
):
    rows, half = tok_hbm.shape
    ep, c = lax.axis_index("ep"), lax.axis_index("tp")
    g, j = ep // 2, ep % 2
    other = {"ep": g * 2 + (1 - j)}
    core = {"tp": 1 - c}
    cut = cap // 2

    operands = (tok_hbm, gain_hbm, ids_hbm, comb_hbm, fgain_hbm)
    staged = (tok_ref, gain_ref, ids_ref, comb_ref, fgain_ref)
    fetches = [
        pltpu.make_async_copy(src, dst, fetch_s.at[i])
        for i, (src, dst) in enumerate(zip(operands, staged))
    ]
    for fetch in fetches:
        fetch.start()

    def flip(a, d):
        return (a % 2 + d % 2) % 2 + 2 * ((a // 2 + d // 2) % 2)

    def plane(d):
        return {"ep": flip(g, d) * 2 + j}

    barrier = pltpu.get_barrier_semaphore()
    for dev in [core, other] + [plane(d) for d in range(1, G)]:
        pl.semaphore_signal(barrier, inc=1, device_id=dev, device_id_type=MESH)

    loads = []
    for i, h in enumerate((c, 1 - c)):
        at = pl.ds(pl.multiple_of(h * half, half), half)
        loads.append(pltpu.make_async_copy(wg_hbm.at[0, at, :], wg.at[i], wsem.at[i]))
        loads.append(pltpu.make_async_copy(wu_hbm.at[0, at, :], wu.at[i], wsem.at[2 + i]))
        loads.append(pltpu.make_async_copy(wd_hbm.at[0, :, at], wd.at[i], wsem.at[4 + i]))

    sent = []

    def send(src, dst, s, r, dev):
        copy = pltpu.make_async_remote_copy(
            src_ref=src, dst_ref=dst, send_sem=s, recv_sem=r, device_id=dev, device_id_type=MESH
        )
        copy.start()
        sent.append(copy)
        return copy

    fetches[2].wait()
    fetches[3].wait()
    group = ids_ref[0:1, :] // 2
    slot8 = lax.broadcasted_iota(jnp.int32, (8, rows), 0)
    onehot = (slot8 == group).astype(f32)
    up_to = lax.broadcasted_iota(jnp.int32, (rows, rows), 0) <= lax.broadcasted_iota(
        jnp.int32, (rows, rows), 1
    )
    counted = jnp.dot(onehot.astype(bf16), up_to.astype(f32).astype(bf16), preferred_element_type=f32)
    rank = jnp.sum(onehot * counted, axis=0, keepdims=True) - 1.0
    offset = flip(group, g)
    target = offset * cap + rank.astype(jnp.int32)
    first = ids_ref[0:1, :] % 2 == 0
    c0, c1 = comb_ref[0:1, :], comb_ref[1:2, :]
    table = jnp.where(slot8 == 0, jnp.where(first, c0, c1), 0.0)
    table = jnp.where(slot8 == 1, jnp.where(first, c1, c0), table)
    table = jnp.where(slot8 == 2, rank, table)
    table = jnp.where(slot8 == 3, group.astype(f32), table)
    pick = (lax.broadcasted_iota(jnp.int32, (G * cap, rows), 0) == target).astype(f32).astype(bf16)
    eye = lax.broadcasted_iota(jnp.int32, (rows, rows), 0) == lax.broadcasted_iota(
        jnp.int32, (rows, rows), 1
    )

    def gather(d):
        return jnp.dot(
            pick[d * cap : (d + 1) * cap], tok_ref[...], preferred_element_type=f32
        ).astype(bf16).reshape(2, cut, half)

    fetches[0].wait()
    sbuf[0] = gather(0)
    sbuf[1] = gather(1)
    sbuf[3] = gather(3)
    x = tok_ref[...].astype(f32)
    sq[0] = fold(x)

    O0, O1, N0, N1, F1, F2, F3, F4 = [
        (0, 0), (0, 1), (1, 0), (1, 1), (3, 0), (2, 0), (3, 1), (2, 1)
    ]
    zs, xs, ts, fs, ps, es, hs = ({} for _ in range(7))

    def depart(u):
        d, r = u
        zs[u] = send(sbuf.at[d, r], rawx.at[d, r], z_s.at[d, r], z_r.at[d, r], plane(d))

    pl.semaphore_wait(barrier, 1 + G)
    xs[O0] = send(sbuf.at[0, 0], rawx.at[0, 0], x_s.at[0, 0], x_r.at[0, 0], other)
    depart(N0)
    first_sq = send(sq.at[0], sq.at[1], sq_s.at[0], sq_r.at[0], core)
    sbuf[2] = gather(2)
    first_sq.wait_recv()
    total = jnp.sum(sq[0] + sq[1], axis=1, keepdims=True)
    scale = lax.rsqrt(total / (2 * half) + EPS)
    across = jnp.sum(jnp.where(eye, scale, 0.0), axis=0, keepdims=True)
    meta[0] = jnp.where(slot8 == 4, across, table)
    metas = {
        d: send(meta.at[0], meta.at[d], m_s.at[d], m_r.at[d], plane(d)) for d in (1, 3, 2)
    }
    metas[G] = send(meta.at[0], meta.at[G], m_s.at[G], m_r.at[G], other)
    xs[O1] = send(sbuf.at[0, 1], rawx.at[0, 1], x_s.at[0, 1], x_r.at[0, 1], other)
    for load in loads:
        load.start()
    fetches[1].wait()
    fetches[4].wait()
    gain = gain_ref[...].astype(f32)[None, :]
    waited = set()

    def sloted(d, r, *names):
        if d and d not in waited:
            waited.add(d)
            metas[d].wait_recv()
        tab = meta[d]
        slots = lax.broadcasted_iota(jnp.int32, (cut, rows), 0) + r * cut
        here = (tab[2:3].astype(jnp.int32) == slots) & (tab[3:4].astype(jnp.int32) == g)
        return [jnp.sum(jnp.where(here, name(tab), 0.0), axis=1, keepdims=True) for name in names]

    def normed(raw, d, r):
        (by,) = sloted(d, r, lambda tab: tab[4:5])
        return (raw.astype(f32) * by * gain).astype(bf16)

    def dispatch(u):
        d, r = u
        mine = xbuf.at[0, d, r, 0]
        if d:
            zs[u].wait_recv()
            xbuf[0, d, r, 0] = normed(rawx[d, r], d, r)
            xs[u] = send(mine, xbuf.at[0, d, r, 1], x_s.at[d, r], x_r.at[d, r], other)
        else:
            xbuf[0, d, r, 0] = normed(sbuf[0, r], 0, r)
        ts[u] = send(mine, xbuf.at[1, d, r, 0], t_s.at[d, r, 0], t_r.at[d, r, 0], core)

    def forward(u):
        d, r = u
        xs[u].wait_recv()
        if d == 0:
            xbuf[0, 0, r, 1] = normed(rawx[0, r], G, r)
        fs[u] = send(
            xbuf.at[0, d, r, 1], xbuf.at[1, d, r, 1], t_s.at[d, r, 1], t_r.at[d, r, 1], core
        )

    def compute(u):
        d, r = u
        ts[u].wait_recv()
        fs[u].wait_recv()
        a = xbuf[0, d, r].reshape(2 * cut, half)
        b = xbuf[1, d, r].reshape(2 * cut, half)
        gate = jnp.dot(a, wg[0], preferred_element_type=f32) + jnp.dot(
            b, wg[1], preferred_element_type=f32
        )
        upper = jnp.dot(a, wu[0], preferred_element_type=f32) + jnp.dot(
            b, wu[1], preferred_element_type=f32
        )
        hidden = (gate / (1.0 + jnp.exp(-gate)) * upper).astype(bf16)
        away = jnp.dot(hidden, wd[1], preferred_element_type=f32)
        psend[d, r] = away.astype(bf16).reshape(2, cut, half)
        ps[u] = send(psend.at[d, r], precv.at[d, r], p_s.at[d, r], p_r.at[d, r], core)
        home = jnp.dot(hidden, wd[0], preferred_element_type=f32)
        pown[d, r] = home.astype(bf16).reshape(2, cut, half)

    def summed(u):
        d, r = u
        ps[u].wait_recv()
        ebuf[d, r, 1] = (pown[d, r, 1].astype(f32) + precv[d, r, 1].astype(f32)).astype(bf16)
        es[u] = send(ebuf.at[d, r, 1], xret.at[d, r], e_s.at[d, r], e_r.at[d, r], other)
        ebuf[d, r, 0] = (pown[d, r, 0].astype(f32) + precv[d, r, 0].astype(f32)).astype(bf16)

    def mix(u):
        d, r = u
        mine, theirs = sloted(
            d, r,
            lambda tab: jnp.where(j == 0, tab[0:1], tab[1:2]),
            lambda tab: jnp.where(j == 0, tab[1:2], tab[0:1]),
        )
        es[u].wait_recv()
        value = (mine * ebuf[d, r, 0].astype(f32) + theirs * xret[d, r].astype(f32)).astype(bf16)
        if d:
            zbuf[d, r] = value
            hs[u] = send(zbuf.at[d, r], ret.at[d, r], h_s.at[d, r], h_r.at[d, r], plane(d))
        else:
            ret[0, r] = value

    back = jnp.sum(jnp.where(eye, target.astype(f32), 0.0), axis=1, keepdims=True).astype(jnp.int32)
    sums = []

    def gathered(u):
        d, r = u
        if d:
            hs[u].wait_recv()
        place = lax.broadcasted_iota(jnp.int32, (rows, cut), 1) + (d * cap + r * cut) == back
        part = jnp.dot(place.astype(f32).astype(bf16), ret[d, r], preferred_element_type=f32)
        acc[...] = acc[...] + part if sums else part
        sums.append(u)

    def arm(u):
        if u == O0:
            for load in loads:
                load.wait()

    schedule = (
        (depart, F1), (dispatch, N0), (depart, N1), (depart, F2), (dispatch, F1),
        (dispatch, N1), (depart, F3), (forward, F1), (forward, N0), (dispatch, O0),
        (dispatch, F2), (arm, O0), (compute, F1), (summed, F1), (forward, O0),
        (depart, F4), (forward, F2), (dispatch, F3), (compute, F2), (compute, O0),
        (summed, F2), (forward, N1), (mix, F1), (forward, F3), (dispatch, F4),
        (dispatch, O1), (compute, N0), (compute, F3), (summed, F3), (summed, N0),
        (mix, F2), (forward, O1), (compute, N1), (forward, F4), (compute, F4),
        (summed, F4), (mix, F3), (summed, N1), (summed, O0), (mix, N0),
        (gathered, F2), (compute, O1), (summed, O1), (gathered, F1), (mix, F4),
        (mix, N1), (mix, O0), (gathered, O0), (gathered, N0), (gathered, F3),
        (gathered, F4), (gathered, N1), (mix, O1), (gathered, O1),
    )
    for step, u in schedule:
        step(u)

    sq[2] = fold(acc[...])
    last_sq = send(sq.at[2], sq.at[3], sq_s.at[1], sq_r.at[1], core)
    last_sq.wait_recv()
    total = jnp.sum(sq[2] + sq[3], axis=1, keepdims=True)
    norm = lax.rsqrt(total / (2 * half) + EPS)
    fgain = fgain_ref[...].astype(f32)[None, :]
    out_ref[...] = (acc[...] * norm * fgain).astype(bf16)
    for copy in sent:
        copy.wait_send()


def paired(tokens, norm_gain, w_gate, w_up, w_down, expert_ids, combine, final_gain):
    rows, half = tokens.shape
    G = lax.axis_size("ep") // 2
    cap = rows // 8 * 5
    ff = w_gate.shape[2]
    hbm = pl.BlockSpec(memory_space=pl.ANY)
    dma = pltpu.SemaphoreType.DMA
    units = (G, 2, cap // 2, half)
    pairs = (G, 2, 2, cap // 2, half)
    return pl.pallas_call(
        functools.partial(paired_kernel, G, cap),
        out_shape=pltpu.VMEM((rows, half), bf16),
        in_specs=[hbm] * 8,
        out_specs=pl.BlockSpec(memory_space=pltpu.VMEM),
        scratch_shapes=[
            pltpu.VMEM((2, half, ff), bf16),
            pltpu.VMEM((2, half, ff), bf16),
            pltpu.VMEM((2, ff, half), bf16),
            pltpu.VMEM((2,) + pairs, bf16),
            pltpu.VMEM(units, bf16),
            pltpu.VMEM(units, bf16),
            pltpu.VMEM((G + 1, 8, rows), f32),
            pltpu.VMEM(pairs, bf16),
            pltpu.VMEM(pairs, bf16),
            pltpu.VMEM(pairs, bf16),
            pltpu.VMEM(pairs, bf16),
            pltpu.VMEM(units, bf16),
            pltpu.VMEM(units, bf16),
            pltpu.VMEM(units, bf16),
            pltpu.VMEM((4, rows, 128), f32),
            pltpu.VMEM((rows, half), f32),
            pltpu.VMEM((rows, half), bf16),
            pltpu.VMEM((half,), bf16),
            pltpu.VMEM((2, rows), jnp.int32),
            pltpu.VMEM((2, rows), f32),
            pltpu.VMEM((half,), bf16),
            dma((5,)), dma((6,)),
            dma((2,)), dma((2,)),
            dma((G, 2)), dma((G, 2)),
            dma((G + 1,)), dma((G + 1,)),
            dma((G, 2)), dma((G, 2)),
            dma((G, 2, 2)), dma((G, 2, 2)),
            dma((G, 2)), dma((G, 2)),
            dma((G, 2)), dma((G, 2)),
            dma((G, 2)), dma((G, 2)),
        ],
        compiler_params=pltpu.CompilerParams(
            collective_id=0, has_side_effects=True, vmem_limit_bytes=57 * 1024 * 1024
        ),
        name="paired",
    )(
        tokens, norm_gain, expert_ids.T, combine.T, final_gain, w_gate, w_up, w_down,
    )


def body(tokens, norm_gain, w_gate, w_up, w_down, expert_ids, combine, final_gain):
    experts = w_gate.shape[0] * lax.axis_size("ep")
    per_group = experts // GROUPS
    args = (tokens, norm_gain, w_gate, w_up, w_down, expert_ids, combine, final_gain)
    if (
        per_group == expert_ids.shape[1] == 2
        and w_gate.shape[0] == 1
        and lax.axis_size("tp") == 2
        and GROUPS == 4
        and tokens.shape[0] % 256 == 0
    ):
        return paired(*args)
    return general(*args)


def solution(mesh):
    placed = (
        P(("grp", "ep"), "tp"),
        P("tp"),
        P("ep", None, "tp"),
        P("ep", None, "tp"),
        P("ep", "tp", None),
        P(("grp", "ep"), None),
        P(("grp", "ep"), None),
        P("tp"),
    )
    return jax.shard_map(
        body, mesh=mesh, in_specs=placed, out_specs=P(("grp", "ep"), "tp"), check_vma=False
    )
```

```python
import functools

import jax
import jax.numpy as jnp
from jax import lax
from jax.experimental import pallas as pl
from jax.experimental.pallas import tpu as pltpu
from jax.sharding import PartitionSpec as P

GROUPS = 4
EPS = 1e-06
MESH = pl.DeviceIdType.MESH
bf16, f32 = jnp.bfloat16, jnp.float32


def general(tokens, norm_gain, w_gate, w_up, w_down, expert_ids, combine, final_gain):
    eps = EPS
    tok_dev, half = tokens.shape
    n_ep = lax.axis_size("ep")
    n_tp = lax.axis_size("tp")
    width = half * n_tp
    exp_dev = w_gate.shape[0]
    experts = exp_dev * n_ep
    per_group = experts // GROUPS
    capacity = tok_dev // 8 * 5 * 2 // per_group
    top = expert_ids.shape[1]
    narrow = tokens.astype(jnp.float32)
    squares = lax.psum(jnp.sum(narrow * narrow, axis=1), "tp")
    scale = lax.rsqrt(squares[:, None] / width + eps)
    normed = (narrow * scale * norm_gain.astype(jnp.float32)).astype(jnp.bfloat16)
    columns = normed.shape[1]
    flat = expert_ids.reshape(-1)
    onehot = (flat[:, None] == jnp.arange(experts, dtype=jnp.int32)[None, :]).astype(jnp.int32)
    ranking = jnp.sum(jnp.cumsum(onehot, axis=0) * onehot, axis=1) - 1
    target = flat * capacity + ranking
    sources = jnp.arange(tok_dev * top, dtype=jnp.int32) // top
    owner = jnp.full((experts * capacity,), tok_dev, jnp.int32).at[target].set(sources)
    padded = jnp.concatenate([normed, jnp.zeros((1, columns), jnp.bfloat16)], axis=0)
    outgoing = padded[owner].reshape(n_ep, exp_dev * capacity, columns)
    arrived = lax.all_to_all(outgoing, "ep", split_axis=0, concat_axis=0, tiled=True)
    rows = (
        arrived.reshape(n_ep, exp_dev, capacity, columns)
        .transpose(1, 0, 2, 3)
        .reshape(exp_dev, n_ep * capacity, columns)
    )
    piece = lax.all_gather(rows, "tp", axis=2, tiled=True)
    gate = jnp.einsum("erd,edf->erf", piece, w_gate, preferred_element_type=jnp.float32)
    upper = jnp.einsum("erd,edf->erf", piece, w_up, preferred_element_type=jnp.float32)
    hidden = (jax.nn.silu(gate) * upper).astype(jnp.bfloat16)
    partial_out = jnp.einsum(
        "erf,efd->erd", hidden, w_down, preferred_element_type=jnp.float32
    ).astype(jnp.bfloat16)
    shares = (
        lax.psum_scatter(partial_out, "tp", scatter_dimension=2, tiled=True)
        .astype(jnp.float32)
        .astype(jnp.bfloat16)
    )
    homeward = (
        shares.reshape(exp_dev, n_ep, capacity, half)
        .transpose(1, 0, 2, 3)
        .reshape(n_ep, exp_dev * capacity, half)
    )
    returned = lax.all_to_all(homeward, "ep", split_axis=0, concat_axis=0, tiled=True).reshape(
        experts * capacity, half
    )
    picked = returned[target].astype(jnp.float32).reshape(tok_dev, top, half)
    mixed = jnp.sum(picked * combine[:, :, None], axis=1)
    totals = lax.psum(jnp.sum(mixed * mixed, axis=1), "tp")
    norm = lax.rsqrt(totals[:, None] / width + eps)
    return (mixed * norm * final_gain.astype(jnp.float32)).astype(jnp.bfloat16)


def fold(v):
    v = v * v
    out = v[:, :128]
    for i in range(1, v.shape[1] // 128):
        out = out + v[:, i * 128 : (i + 1) * 128]
    return out


def paired_kernel(
    G, cap, tok_hbm, gain_hbm, ids_hbm, comb_hbm, fgain_hbm, wg_hbm, wu_hbm, wd_hbm, out_ref,
    wg, wu, wd, xbuf, sbuf, rawx, meta, psend, pown, precv, ebuf, xret, zbuf, ret, sq, acc,
    tok_ref, gain_ref, ids_ref, comb_ref, fgain_ref,
    fetch_s, wsem, sq_s, sq_r, z_s, z_r, m_s, m_r, x_s, x_r, t_s, t_r, p_s, p_r, e_s, e_r,
    h_s, h_r,
):
    rows, half = tok_hbm.shape
    ep, c = lax.axis_index("ep"), lax.axis_index("tp")
    g, j = ep // 2, ep % 2
    other = {"ep": g * 2 + (1 - j)}
    core = {"tp": 1 - c}
    cut = cap // 2

    operands = (tok_hbm, gain_hbm, ids_hbm, comb_hbm, fgain_hbm)
    staged = (tok_ref, gain_ref, ids_ref, comb_ref, fgain_ref)
    fetches = [
        pltpu.make_async_copy(src, dst, fetch_s.at[i])
        for i, (src, dst) in enumerate(zip(operands, staged))
    ]
    for fetch in fetches:
        fetch.start()

    def flip(a, d):
        return (a % 2 + d % 2) % 2 + 2 * ((a // 2 + d // 2) % 2)

    def plane(d):
        return {"ep": flip(g, d) * 2 + j}

    barrier = pltpu.get_barrier_semaphore()

    def greet(dev):
        pl.semaphore_signal(barrier, inc=1, device_id=dev, device_id_type=MESH)

    greet(core)
    greet(other)
    for d in range(1, G):
        pl.when((g != 0) & (g != d))(functools.partial(greet, plane(d)))

    loads = []
    for i, h in enumerate((c, 1 - c)):
        at = pl.ds(pl.multiple_of(h * half, half), half)
        loads.append(pltpu.make_async_copy(wg_hbm.at[0, at, :], wg.at[i], wsem.at[0]))
        loads.append(pltpu.make_async_copy(wu_hbm.at[0, at, :], wu.at[i], wsem.at[1]))
        loads.append(pltpu.make_async_copy(wd_hbm.at[0, :, at], wd.at[i], wsem.at[2]))

    def send(src, dst, s, r, dev):
        copy = pltpu.make_async_remote_copy(
            src_ref=src, dst_ref=dst, send_sem=s, recv_sem=r, device_id=dev, device_id_type=MESH
        )
        copy.start()
        return copy

    fetches[2].wait()
    fetches[3].wait()
    group = ids_ref[0:1, :] // 2
    slot8 = lax.broadcasted_iota(jnp.int32, (8, rows), 0)
    onehot = (slot8 == group).astype(f32)
    up_to = lax.broadcasted_iota(jnp.int32, (rows, rows), 0) <= lax.broadcasted_iota(
        jnp.int32, (rows, rows), 1
    )
    counted = jnp.dot(onehot.astype(bf16), up_to.astype(f32).astype(bf16), preferred_element_type=f32)
    rank = jnp.sum(onehot * counted, axis=0, keepdims=True) - 1.0
    offset = flip(group, g)
    target = offset * cap + rank.astype(jnp.int32)
    first = ids_ref[0:1, :] % 2 == 0
    c0, c1 = comb_ref[0:1, :], comb_ref[1:2, :]
    table = jnp.where(slot8 == 0, jnp.where(first, c0, c1), 0.0)
    table = jnp.where(slot8 == 1, jnp.where(first, c1, c0), table)
    table = jnp.where(slot8 == 2, rank, table)
    table = jnp.where(slot8 == 3, group.astype(f32), table)
    pick = (lax.broadcasted_iota(jnp.int32, (G * cap, rows), 0) == target).astype(f32).astype(bf16)
    eye = lax.broadcasted_iota(jnp.int32, (rows, rows), 0) == lax.broadcasted_iota(
        jnp.int32, (rows, rows), 1
    )

    def across(column):
        return jnp.where(slot8 == 0, jnp.sum(jnp.where(eye, column, 0.0), axis=0, keepdims=True), 0.0)

    def gather(d):
        return jnp.dot(
            pick[d * cap : (d + 1) * cap], tok_ref[...], preferred_element_type=f32
        ).astype(bf16).reshape(2, cut, half)

    fetches[0].wait()
    sbuf[0] = gather(0)
    O0, O1, N0, N1, F1, F2, F3, F4 = [
        (0, 0), (0, 1), (1, 0), (1, 1), (3, 0), (2, 0), (3, 1), (2, 1)
    ]
    zs, xs, ts, fs, ps, es, hs = ({} for _ in range(7))

    @pl.when(g == 0)
    def _():
        pl.semaphore_wait(barrier, 2)
        for d in range(1, G):
            greet(plane(d))

    @pl.when(g != 0)
    def _():
        pl.semaphore_wait(barrier, 1 + G)
        greet({"ep": j})

    def depart(u):
        d, r = u
        zs[u] = send(sbuf.at[d, r], rawx.at[d, r], z_s, z_r.at[d - 1, r], plane(d))

    xs[O0] = send(sbuf.at[0, 0], rawx.at[0, 0], x_s, x_r.at[0, 0], other)
    sbuf[1] = gather(1)
    zs[N0] = pltpu.make_async_remote_copy(
        src_ref=sbuf.at[1, 0], dst_ref=rawx.at[1, 0], send_sem=z_s, recv_sem=z_r.at[0, 0],
        device_id=plane(1), device_id_type=MESH,
    )
    pl.when(g != 0)(zs[N0].start)
    sq[0] = across(jnp.sum(fold(tok_ref[...].astype(f32)), axis=1, keepdims=True))
    first_sq = send(sq.at[0], sq.at[1], sq_s.at[0], sq_r.at[0], core)
    sbuf[3] = gather(3)
    sbuf[2] = gather(2)
    first_sq.wait_recv()
    scale = lax.rsqrt((sq[0, 0:1] + sq[1, 0:1]) / (2 * half) + EPS)
    meta[0] = jnp.where(slot8 == 4, scale, table)
    metas = {G: send(meta.at[0], meta.at[G], m_s, m_r.at[G - 1], other)}
    xs[O1] = send(sbuf.at[0, 1], rawx.at[0, 1], x_s, x_r.at[0, 1], other)

    @pl.when(g == 0)
    def _():
        pl.semaphore_wait(barrier, G - 1)
        zs[N0].start()

    for d in (1, 3, 2):
        metas[d] = send(meta.at[0], meta.at[d], m_s, m_r.at[d - 1], plane(d))
    for load in loads:
        load.start()
    fetches[1].wait()
    fetches[4].wait()
    gain = gain_ref[...].astype(f32)[None, :]
    waited = set()

    def sloted(d, r, *names):
        if d and d not in waited:
            waited.add(d)
            metas[d].wait_recv()
        tab = meta[d]
        slots = lax.broadcasted_iota(jnp.int32, (cut, rows), 0) + r * cut
        here = (tab[2:3].astype(jnp.int32) == slots) & (tab[3:4].astype(jnp.int32) == g)
        return [jnp.sum(jnp.where(here, name(tab), 0.0), axis=1, keepdims=True) for name in names]

    def normed(raw, d, r):
        (by,) = sloted(d, r, lambda tab: tab[4:5])
        return (raw.astype(f32) * by * gain).astype(bf16)

    def dispatch(u):
        d, r = u
        mine = xbuf.at[0, d, r, 0]
        if d:
            zs[u].wait_recv()
            xbuf[0, d, r, 0] = normed(rawx[d, r], d, r)
            xs[u] = send(mine, xbuf.at[0, d, r, 1], x_s, x_r.at[d, r], other)
        else:
            xbuf[0, d, r, 0] = normed(sbuf[0, r], 0, r)
        ts[u] = send(mine, xbuf.at[1, d, r, 0], t_s.at[0], t_r.at[d, r], core)

    def forward(u):
        d, r = u
        xs[u].wait_recv()
        if d == 0:
            xbuf[0, 0, r, 1] = normed(rawx[0, r], G, r)
        fs[u] = send(
            xbuf.at[0, d, r, 1], xbuf.at[1, d, r, 1], t_s.at[1], t_r.at[d, r], core
        )

    def compute(u):
        d, r = u
        whole = xbuf.at[1, d, r]
        pltpu.make_async_copy(whole, whole, t_r.at[d, r]).wait()
        a = xbuf[0, d, r].reshape(2 * cut, half)
        b = xbuf[1, d, r].reshape(2 * cut, half)
        gate = jnp.dot(a, wg[0], preferred_element_type=f32) + jnp.dot(
            b, wg[1], preferred_element_type=f32
        )
        upper = jnp.dot(a, wu[0], preferred_element_type=f32) + jnp.dot(
            b, wu[1], preferred_element_type=f32
        )
        hidden = (gate / (1.0 + jnp.exp(-gate)) * upper).astype(bf16)
        away = jnp.dot(hidden, wd[1], preferred_element_type=f32)
        psend[d, r] = away.astype(bf16).reshape(2, cut, half)
        ps[u] = send(psend.at[d, r], precv.at[d, r], p_s, p_r.at[d, r], core)
        home = jnp.dot(hidden, wd[0], preferred_element_type=f32)
        pown[d, r] = home.astype(bf16).reshape(2, cut, half)

    def summed(u):
        d, r = u
        ps[u].wait_recv()
        ebuf[d, r, 1] = (pown[d, r, 1].astype(f32) + precv[d, r, 1].astype(f32)).astype(bf16)
        es[u] = send(ebuf.at[d, r, 1], xret.at[d, r], e_s, e_r.at[d, r], other)
        ebuf[d, r, 0] = (pown[d, r, 0].astype(f32) + precv[d, r, 0].astype(f32)).astype(bf16)

    def mix(u):
        d, r = u
        mine, theirs = sloted(
            d, r,
            lambda tab: jnp.where(j == 0, tab[0:1], tab[1:2]),
            lambda tab: jnp.where(j == 0, tab[1:2], tab[0:1]),
        )
        es[u].wait_recv()
        value = (mine * ebuf[d, r, 0].astype(f32) + theirs * xret[d, r].astype(f32)).astype(bf16)
        if d:
            zbuf[d, r] = value
            hs[u] = send(zbuf.at[d, r], ret.at[d, r], h_s, h_r.at[d - 1, r], plane(d))
        else:
            ret[0, r] = value

    back = jnp.sum(jnp.where(eye, target.astype(f32), 0.0), axis=1, keepdims=True).astype(jnp.int32)
    sums = []

    def gathered(u):
        d, r = u
        if d:
            hs[u].wait_recv()
        place = lax.broadcasted_iota(jnp.int32, (rows, cut), 1) + (d * cap + r * cut) == back
        part = jnp.dot(place.astype(f32).astype(bf16), ret[d, r], preferred_element_type=f32)
        acc[...] = acc[...] + part if sums else part
        sums.append(u)

    def arm(u):
        if u == O0:
            for i, ref in enumerate((wg, wu, wd)):
                pltpu.make_async_copy(ref, ref, wsem.at[i]).wait()

    schedule = (
        (dispatch, O0), (depart, F1), (depart, N1), (depart, F2), (dispatch, N0),
        (dispatch, F1), (forward, N0), (dispatch, N1), (depart, F3), (arm, O0),
        (compute, N0), (summed, N0), (dispatch, F2), (forward, F1), (compute, F1),
        (depart, F4), (forward, N1), (mix, N0), (dispatch, O1), (summed, F1),
        (dispatch, F3), (forward, F2), (compute, N1), (compute, F2), (summed, F2),
        (mix, F1), (forward, F3), (dispatch, F4), (compute, F3), (summed, F3),
        (forward, O0), (summed, N1), (mix, F2), (forward, F4), (compute, F4),
        (forward, O1), (mix, F3), (summed, F4), (compute, O1), (summed, O1),
        (gathered, F2), (mix, N1), (compute, O0), (gathered, N0), (summed, O0),
        (gathered, F1), (mix, F4), (gathered, F3), (mix, O1), (gathered, O1),
        (gathered, N1), (mix, O0), (gathered, O0), (gathered, F4),
    )
    for step, u in schedule:
        step(u)

    sq[2] = across(jnp.sum(fold(acc[...]), axis=1, keepdims=True))
    last_sq = send(sq.at[2], sq.at[3], sq_s.at[1], sq_r.at[1], core)
    last_sq.wait_recv()
    norm = lax.rsqrt((sq[2, 0:1] + sq[3, 0:1]) / (2 * half) + EPS)
    norm = jnp.sum(jnp.where(eye, norm, 0.0), axis=1, keepdims=True)
    fgain = fgain_ref[...].astype(f32)[None, :]
    out_ref[...] = (acc[...] * norm * fgain).astype(bf16)
    drains = [
        (sbuf.at[1:G], z_s), (meta.at[1 : G + 1], m_s), (sbuf, x_s), (sbuf, t_s.at[0]),
        (sbuf, t_s.at[1]), (psend, p_s), (sbuf, e_s), (zbuf.at[1:G], h_s),
        (sq.at[0], sq_s.at[0]), (sq.at[2], sq_s.at[1]),
    ]
    for ref, sem in drains:
        pltpu.make_async_copy(ref, ref, sem).wait()


def paired(tokens, norm_gain, w_gate, w_up, w_down, expert_ids, combine, final_gain):
    rows, half = tokens.shape
    G = lax.axis_size("ep") // 2
    cap = rows // 8 * 5
    ff = w_gate.shape[2]
    hbm = pl.BlockSpec(memory_space=pl.ANY)
    dma = pltpu.SemaphoreType.DMA
    units = (G, 2, cap // 2, half)
    pairs = (G, 2, 2, cap // 2, half)
    return pl.pallas_call(
        functools.partial(paired_kernel, G, cap),
        out_shape=pltpu.VMEM((rows, half), bf16),
        in_specs=[hbm] * 8,
        out_specs=pl.BlockSpec(memory_space=pltpu.VMEM),
        scratch_shapes=[
            pltpu.VMEM((2, half, ff), bf16),
            pltpu.VMEM((2, half, ff), bf16),
            pltpu.VMEM((2, ff, half), bf16),
            pltpu.VMEM((2,) + pairs, bf16),
            pltpu.VMEM(units, bf16),
            pltpu.VMEM(units, bf16),
            pltpu.VMEM((G + 1, 8, rows), f32),
            pltpu.VMEM(pairs, bf16),
            pltpu.VMEM(pairs, bf16),
            pltpu.VMEM(pairs, bf16),
            pltpu.VMEM(pairs, bf16),
            pltpu.VMEM(units, bf16),
            pltpu.VMEM(units, bf16),
            pltpu.VMEM(units, bf16),
            pltpu.VMEM((4, 8, rows), f32),
            pltpu.VMEM((rows, half), f32),
            pltpu.VMEM((rows, half), bf16),
            pltpu.VMEM((half,), bf16),
            pltpu.VMEM((2, rows), jnp.int32),
            pltpu.VMEM((2, rows), f32),
            pltpu.VMEM((half,), bf16),
            dma((5,)), dma((3,)),
            dma((2,)), dma((2,)),
            dma, dma((G - 1, 2)),
            dma, dma((G,)),
            dma, dma((G, 2)),
            dma((2,)), dma((G, 2)),
            dma, dma((G, 2)),
            dma, dma((G, 2)),
            dma, dma((G - 1, 2)),
        ],
        compiler_params=pltpu.CompilerParams(
            collective_id=0, has_side_effects=True, vmem_limit_bytes=57 * 1024 * 1024
        ),
        name="paired",
    )(
        tokens, norm_gain, expert_ids.T, combine.T, final_gain, w_gate, w_up, w_down,
    )


def body(tokens, norm_gain, w_gate, w_up, w_down, expert_ids, combine, final_gain):
    experts = w_gate.shape[0] * lax.axis_size("ep")
    per_group = experts // GROUPS
    args = (tokens, norm_gain, w_gate, w_up, w_down, expert_ids, combine, final_gain)
    if (
        per_group == expert_ids.shape[1] == 2
        and w_gate.shape[0] == 1
        and lax.axis_size("tp") == 2
        and GROUPS == 4
        and tokens.shape[0] % 256 == 0
    ):
        return paired(*args)
    return general(*args)


def solution(mesh):
    placed = (
        P(("grp", "ep"), "tp"),
        P("tp"),
        P("ep", None, "tp"),
        P("ep", None, "tp"),
        P("ep", "tp", None),
        P(("grp", "ep"), None),
        P(("grp", "ep"), None),
        P("tp"),
    )
    return jax.shard_map(
        body, mesh=mesh, in_specs=placed, out_specs=P(("grp", "ep"), "tp"), check_vma=False
    )
```

```python
import functools

import jax
import jax.numpy as jnp
from jax import lax
from jax.experimental import pallas as pl
from jax.experimental.pallas import tpu as pltpu
from jax.sharding import PartitionSpec as P

GROUPS = 4
EPS = 1e-06
MESH = pl.DeviceIdType.MESH
bf16, f32 = jnp.bfloat16, jnp.float32


def general(tokens, norm_gain, w_gate, w_up, w_down, expert_ids, combine, final_gain):
    eps = EPS
    tok_dev, half = tokens.shape
    n_ep = lax.axis_size("ep")
    n_tp = lax.axis_size("tp")
    width = half * n_tp
    exp_dev = w_gate.shape[0]
    experts = exp_dev * n_ep
    per_group = experts // GROUPS
    capacity = tok_dev // 8 * 5 * 2 // per_group
    top = expert_ids.shape[1]
    narrow = tokens.astype(jnp.float32)
    squares = lax.psum(jnp.sum(narrow * narrow, axis=1), "tp")
    scale = lax.rsqrt(squares[:, None] / width + eps)
    normed = (narrow * scale * norm_gain.astype(jnp.float32)).astype(jnp.bfloat16)
    columns = normed.shape[1]
    flat = expert_ids.reshape(-1)
    onehot = (flat[:, None] == jnp.arange(experts, dtype=jnp.int32)[None, :]).astype(jnp.int32)
    ranking = jnp.sum(jnp.cumsum(onehot, axis=0) * onehot, axis=1) - 1
    target = flat * capacity + ranking
    sources = jnp.arange(tok_dev * top, dtype=jnp.int32) // top
    owner = jnp.full((experts * capacity,), tok_dev, jnp.int32).at[target].set(sources)
    padded = jnp.concatenate([normed, jnp.zeros((1, columns), jnp.bfloat16)], axis=0)
    outgoing = padded[owner].reshape(n_ep, exp_dev * capacity, columns)
    arrived = lax.all_to_all(outgoing, "ep", split_axis=0, concat_axis=0, tiled=True)
    rows = (
        arrived.reshape(n_ep, exp_dev, capacity, columns)
        .transpose(1, 0, 2, 3)
        .reshape(exp_dev, n_ep * capacity, columns)
    )
    piece = lax.all_gather(rows, "tp", axis=2, tiled=True)
    gate = jnp.einsum("erd,edf->erf", piece, w_gate, preferred_element_type=jnp.float32)
    upper = jnp.einsum("erd,edf->erf", piece, w_up, preferred_element_type=jnp.float32)
    hidden = (jax.nn.silu(gate) * upper).astype(jnp.bfloat16)
    partial_out = jnp.einsum(
        "erf,efd->erd", hidden, w_down, preferred_element_type=jnp.float32
    ).astype(jnp.bfloat16)
    shares = (
        lax.psum_scatter(partial_out, "tp", scatter_dimension=2, tiled=True)
        .astype(jnp.float32)
        .astype(jnp.bfloat16)
    )
    homeward = (
        shares.reshape(exp_dev, n_ep, capacity, half)
        .transpose(1, 0, 2, 3)
        .reshape(n_ep, exp_dev * capacity, half)
    )
    returned = lax.all_to_all(homeward, "ep", split_axis=0, concat_axis=0, tiled=True).reshape(
        experts * capacity, half
    )
    picked = returned[target].astype(jnp.float32).reshape(tok_dev, top, half)
    mixed = jnp.sum(picked * combine[:, :, None], axis=1)
    totals = lax.psum(jnp.sum(mixed * mixed, axis=1), "tp")
    norm = lax.rsqrt(totals[:, None] / width + eps)
    return (mixed * norm * final_gain.astype(jnp.float32)).astype(jnp.bfloat16)


def fold(v):
    v = v * v
    out = v[:, :128]
    for i in range(1, v.shape[1] // 128):
        out = out + v[:, i * 128 : (i + 1) * 128]
    return out


def paired_kernel(
    G, cap, tok_hbm, gain_hbm, ids_hbm, comb_hbm, fgain_hbm, wg_hbm, wu_hbm, wd_hbm, out_ref,
    wg, wu, wd, xbuf, sbuf, rawx, meta, psend, pown, precv, ebuf, xret, zbuf, ret, sq, acc,
    tok_ref, gain_ref, ids_ref, comb_ref, fgain_ref,
    fetch_s, wsem, sq_s, sq_r, z_s, z_r, m_s, m_r, x_s, x_r, t_s, t_r, p_s, p_r, e_s, e_r,
    h_s, h_r,
):
    rows, half = tok_hbm.shape
    ep, c = lax.axis_index("ep"), lax.axis_index("tp")
    g, j = ep // 2, ep % 2
    other = {"ep": g * 2 + (1 - j)}
    core = {"tp": 1 - c}
    cut = cap // 2

    operands = (tok_hbm, gain_hbm, ids_hbm, comb_hbm, fgain_hbm)
    staged = (tok_ref, gain_ref, ids_ref, comb_ref, fgain_ref)
    fetches = [
        pltpu.make_async_copy(src, dst, fetch_s.at[i])
        for i, (src, dst) in enumerate(zip(operands, staged))
    ]
    for fetch in fetches:
        fetch.start()

    def flip(a, d):
        return (a % 2 + d % 2) % 2 + 2 * ((a // 2 + d // 2) % 2)

    def plane(d):
        return {"ep": flip(g, d) * 2 + j}

    barrier = pltpu.get_barrier_semaphore()

    def greet(dev):
        pl.semaphore_signal(barrier, inc=1, device_id=dev, device_id_type=MESH)

    greet(core)
    greet(other)
    for d in range(1, G):
        pl.when((g != 0) & (g != d))(functools.partial(greet, plane(d)))

    loads = []
    for i, h in enumerate((c, 1 - c)):
        at = pl.ds(pl.multiple_of(h * half, half), half)
        loads.append(pltpu.make_async_copy(wg_hbm.at[0, at, :], wg.at[i], wsem.at[0]))
        loads.append(pltpu.make_async_copy(wu_hbm.at[0, at, :], wu.at[i], wsem.at[1]))
        loads.append(pltpu.make_async_copy(wd_hbm.at[0, :, at], wd.at[i], wsem.at[2]))

    def send(src, dst, s, r, dev):
        copy = pltpu.make_async_remote_copy(
            src_ref=src, dst_ref=dst, send_sem=s, recv_sem=r, device_id=dev, device_id_type=MESH
        )
        copy.start()
        return copy

    fetches[2].wait()
    fetches[3].wait()
    group = ids_ref[0:1, :] // 2
    slot8 = lax.broadcasted_iota(jnp.int32, (8, rows), 0)
    onehot = (slot8 == group).astype(f32)
    up_to = lax.broadcasted_iota(jnp.int32, (rows, rows), 0) <= lax.broadcasted_iota(
        jnp.int32, (rows, rows), 1
    )
    counted = jnp.dot(onehot.astype(bf16), up_to.astype(f32).astype(bf16), preferred_element_type=f32)
    rank = jnp.sum(onehot * counted, axis=0, keepdims=True) - 1.0
    offset = flip(group, g)
    target = offset * cap + rank.astype(jnp.int32)
    first = ids_ref[0:1, :] % 2 == 0
    c0, c1 = comb_ref[0:1, :], comb_ref[1:2, :]
    table = jnp.where(slot8 == 0, jnp.where(first, c0, c1), 0.0)
    table = jnp.where(slot8 == 1, jnp.where(first, c1, c0), table)
    table = jnp.where(slot8 == 2, rank, table)
    table = jnp.where(slot8 == 3, group.astype(f32), table)
    pick = (lax.broadcasted_iota(jnp.int32, (G * cap, rows), 0) == target).astype(f32).astype(bf16)
    eye = lax.broadcasted_iota(jnp.int32, (rows, rows), 0) == lax.broadcasted_iota(
        jnp.int32, (rows, rows), 1
    )

    def across(column):
        return jnp.where(slot8 == 0, jnp.sum(jnp.where(eye, column, 0.0), axis=0, keepdims=True), 0.0)

    def gather(d):
        return jnp.dot(
            pick[d * cap : (d + 1) * cap], tok_ref[...], preferred_element_type=f32
        ).astype(bf16).reshape(2, cut, half)

    fetches[0].wait()
    sbuf[0] = gather(0)
    O0, O1, N0, N1, F1, F2, F3, F4 = [
        (0, 0), (0, 1), (1, 0), (1, 1), (3, 0), (2, 0), (3, 1), (2, 1)
    ]
    zs, xs, ts, fs, ps, es, hs = ({} for _ in range(7))

    @pl.when(g == 0)
    def _():
        pl.semaphore_wait(barrier, 2)
        for d in range(1, G):
            greet(plane(d))

    @pl.when(g != 0)
    def _():
        pl.semaphore_wait(barrier, 1 + G)
        greet({"ep": j})

    def depart(u):
        d, r = u
        zs[u] = send(sbuf.at[d, r], rawx.at[d, r], z_s, z_r.at[d - 1, r], plane(d))

    xs[O0] = send(sbuf.at[0, 0], rawx.at[0, 0], x_s, x_r.at[0, 0], other)
    sbuf[1] = gather(1)
    zs[N0] = pltpu.make_async_remote_copy(
        src_ref=sbuf.at[1, 0], dst_ref=rawx.at[1, 0], send_sem=z_s, recv_sem=z_r.at[0, 0],
        device_id=plane(1), device_id_type=MESH,
    )
    pl.when(g != 0)(zs[N0].start)
    sq[0] = across(jnp.sum(fold(tok_ref[...].astype(f32)), axis=1, keepdims=True))
    first_sq = send(sq.at[0], sq.at[1], sq_s.at[0], sq_r.at[0], core)
    sbuf[3] = gather(3)
    sbuf[2] = gather(2)
    first_sq.wait_recv()
    scale = lax.rsqrt((sq[0, 0:1] + sq[1, 0:1]) / (2 * half) + EPS)
    meta[0] = jnp.where(slot8 == 4, scale, table)
    metas = {G: send(meta.at[0], meta.at[G], m_s, m_r.at[G - 1], other)}
    xs[O1] = send(sbuf.at[0, 1], rawx.at[0, 1], x_s, x_r.at[0, 1], other)

    @pl.when(g == 0)
    def _():
        pl.semaphore_wait(barrier, G - 1)
        zs[N0].start()

    for d in (1, 3, 2):
        metas[d] = send(meta.at[0], meta.at[d], m_s, m_r.at[d - 1], plane(d))
    for load in loads:
        load.start()
    fetches[1].wait()
    fetches[4].wait()
    gain = gain_ref[...].astype(f32)[None, :]
    waited = set()

    def sloted(d, r, *names):
        if d and d not in waited:
            waited.add(d)
            metas[d].wait_recv()
        tab = meta[d]
        slots = lax.broadcasted_iota(jnp.int32, (cut, rows), 0) + r * cut
        here = (tab[2:3].astype(jnp.int32) == slots) & (tab[3:4].astype(jnp.int32) == g)
        return [jnp.sum(jnp.where(here, name(tab), 0.0), axis=1, keepdims=True) for name in names]

    def normed(raw, d, r):
        (by,) = sloted(d, r, lambda tab: tab[4:5])
        return (raw.astype(f32) * by * gain).astype(bf16)

    def dispatch(u):
        d, r = u
        mine = xbuf.at[0, d, r, 0]
        if d:
            zs[u].wait_recv()
            xbuf[0, d, r, 0] = normed(rawx[d, r], d, r)
            xs[u] = send(mine, xbuf.at[0, d, r, 1], x_s, x_r.at[d, r], other)
        else:
            xbuf[0, d, r, 0] = normed(sbuf[0, r], 0, r)
        ts[u] = send(mine, xbuf.at[1, d, r, 0], t_s.at[0], t_r.at[d, r], core)

    def forward(u):
        d, r = u
        xs[u].wait_recv()
        if d == 0:
            xbuf[0, 0, r, 1] = normed(rawx[0, r], G, r)
        fs[u] = send(
            xbuf.at[0, d, r, 1], xbuf.at[1, d, r, 1], t_s.at[1], t_r.at[d, r], core
        )

    def compute(u):
        d, r = u
        whole = xbuf.at[1, d, r]
        pltpu.make_async_copy(whole, whole, t_r.at[d, r]).wait()
        a = xbuf[0, d, r].reshape(2 * cut, half)
        b = xbuf[1, d, r].reshape(2 * cut, half)
        gate = jnp.dot(a, wg[0], preferred_element_type=f32) + jnp.dot(
            b, wg[1], preferred_element_type=f32
        )
        upper = jnp.dot(a, wu[0], preferred_element_type=f32) + jnp.dot(
            b, wu[1], preferred_element_type=f32
        )
        hidden = (gate / (1.0 + jnp.exp(-gate)) * upper).astype(bf16)
        away = jnp.dot(hidden, wd[1], preferred_element_type=f32)
        psend[d, r] = away.astype(bf16).reshape(2, cut, half)
        ps[u] = send(psend.at[d, r], precv.at[d, r], p_s, p_r.at[d, r], core)
        home = jnp.dot(hidden, wd[0], preferred_element_type=f32)
        pown[d, r] = home.astype(bf16).reshape(2, cut, half)

    def summed(u):
        d, r = u
        ps[u].wait_recv()
        ebuf[d, r, 1] = (pown[d, r, 1].astype(f32) + precv[d, r, 1].astype(f32)).astype(bf16)
        es[u] = send(ebuf.at[d, r, 1], xret.at[d, r], e_s, e_r.at[d, r], other)
        ebuf[d, r, 0] = (pown[d, r, 0].astype(f32) + precv[d, r, 0].astype(f32)).astype(bf16)

    def mix(u):
        d, r = u
        mine, theirs = sloted(
            d, r,
            lambda tab: jnp.where(j == 0, tab[0:1], tab[1:2]),
            lambda tab: jnp.where(j == 0, tab[1:2], tab[0:1]),
        )
        es[u].wait_recv()
        value = (mine * ebuf[d, r, 0].astype(f32) + theirs * xret[d, r].astype(f32)).astype(bf16)
        if d:
            zbuf[d, r] = value
            hs[u] = send(zbuf.at[d, r], ret.at[d, r], h_s, h_r.at[d - 1, r], plane(d))
        else:
            ret[0, r] = value

    back = jnp.sum(jnp.where(eye, target.astype(f32), 0.0), axis=1, keepdims=True).astype(jnp.int32)
    sums = []

    squares = []
    last_sq = []

    def gathered(u):
        d, r = u
        if d:
            hs[u].wait_recv()
        start = d * cap + r * cut
        held = jnp.sum(fold(ret[d, r].astype(f32)), axis=1, keepdims=True)
        at = lax.broadcasted_iota(jnp.int32, (cut, rows), 0) + start == target
        squares.append(jnp.sum(jnp.where(at, held, 0.0), axis=0, keepdims=True))
        if len(squares) == 2 * G:
            sq[2] = jnp.where(slot8 == 0, sum(squares[1:], squares[0]), 0.0)
            last_sq.append(send(sq.at[2], sq.at[3], sq_s.at[1], sq_r.at[1], core))
        place = lax.broadcasted_iota(jnp.int32, (rows, cut), 1) + start == back
        part = jnp.dot(place.astype(f32).astype(bf16), ret[d, r], preferred_element_type=f32)
        acc[...] = acc[...] + part if sums else part
        sums.append(u)

    def arm(u):
        if u == O0:
            for i, ref in enumerate((wg, wu, wd)):
                pltpu.make_async_copy(ref, ref, wsem.at[i]).wait()

    schedule = (
        (depart, F1), (dispatch, O0), (depart, N1), (dispatch, N0), (depart, F2),
        (dispatch, F1), (forward, N0), (dispatch, N1), (depart, F3), (arm, O0),
        (compute, N0), (summed, N0), (dispatch, F2), (forward, F1), (compute, F1),
        (dispatch, O1), (depart, F4), (summed, F1), (forward, N1), (dispatch, F3),
        (mix, N0), (forward, F2), (compute, F2), (summed, F2), (mix, F1),
        (dispatch, F4), (forward, F3), (compute, F3), (gathered, N0), (forward, O0),
        (compute, N1), (summed, F3), (mix, F2), (summed, N1), (forward, F4),
        (compute, O0), (compute, F4), (mix, F3), (summed, F4), (gathered, F2),
        (mix, N1), (summed, O0), (forward, O1), (gathered, F1), (compute, O1),
        (mix, F4), (summed, O1), (mix, O0), (gathered, O0), (gathered, F3),
        (gathered, N1), (mix, O1), (gathered, O1), (gathered, F4),
    )
    for step, u in schedule:
        step(u)

    last_sq[0].wait_recv()
    norm = lax.rsqrt((sq[2, 0:1] + sq[3, 0:1]) / (2 * half) + EPS)
    norm = jnp.sum(jnp.where(eye, norm, 0.0), axis=1, keepdims=True)
    fgain = fgain_ref[...].astype(f32)[None, :]
    out_ref[...] = (acc[...] * norm * fgain).astype(bf16)
    drains = [
        (sbuf.at[1:G], z_s), (meta.at[1 : G + 1], m_s), (sbuf, x_s), (sbuf, t_s.at[0]),
        (sbuf, t_s.at[1]), (psend, p_s), (sbuf, e_s), (zbuf.at[1:G], h_s),
        (sq.at[0], sq_s.at[0]), (sq.at[2], sq_s.at[1]),
    ]
    for ref, sem in drains:
        pltpu.make_async_copy(ref, ref, sem).wait()


def paired(tokens, norm_gain, w_gate, w_up, w_down, expert_ids, combine, final_gain):
    rows, half = tokens.shape
    G = lax.axis_size("ep") // 2
    cap = rows // 8 * 5
    ff = w_gate.shape[2]
    hbm = pl.BlockSpec(memory_space=pl.ANY)
    dma = pltpu.SemaphoreType.DMA
    units = (G, 2, cap // 2, half)
    pairs = (G, 2, 2, cap // 2, half)
    return pl.pallas_call(
        functools.partial(paired_kernel, G, cap),
        out_shape=pltpu.VMEM((rows, half), bf16),
        in_specs=[hbm] * 8,
        out_specs=pl.BlockSpec(memory_space=pltpu.VMEM),
        scratch_shapes=[
            pltpu.VMEM((2, half, ff), bf16),
            pltpu.VMEM((2, half, ff), bf16),
            pltpu.VMEM((2, ff, half), bf16),
            pltpu.VMEM((2,) + pairs, bf16),
            pltpu.VMEM(units, bf16),
            pltpu.VMEM(units, bf16),
            pltpu.VMEM((G + 1, 8, rows), f32),
            pltpu.VMEM(pairs, bf16),
            pltpu.VMEM(pairs, bf16),
            pltpu.VMEM(pairs, bf16),
            pltpu.VMEM(pairs, bf16),
            pltpu.VMEM(units, bf16),
            pltpu.VMEM(units, bf16),
            pltpu.VMEM(units, bf16),
            pltpu.VMEM((4, 8, rows), f32),
            pltpu.VMEM((rows, half), f32),
            pltpu.VMEM((rows, half), bf16),
            pltpu.VMEM((half,), bf16),
            pltpu.VMEM((2, rows), jnp.int32),
            pltpu.VMEM((2, rows), f32),
            pltpu.VMEM((half,), bf16),
            dma((5,)), dma((3,)),
            dma((2,)), dma((2,)),
            dma, dma((G - 1, 2)),
            dma, dma((G,)),
            dma, dma((G, 2)),
            dma((2,)), dma((G, 2)),
            dma, dma((G, 2)),
            dma, dma((G, 2)),
            dma, dma((G - 1, 2)),
        ],
        compiler_params=pltpu.CompilerParams(
            collective_id=0, has_side_effects=True, vmem_limit_bytes=57 * 1024 * 1024
        ),
        name="paired",
    )(
        tokens, norm_gain, expert_ids.T, combine.T, final_gain, w_gate, w_up, w_down,
    )


def body(tokens, norm_gain, w_gate, w_up, w_down, expert_ids, combine, final_gain):
    experts = w_gate.shape[0] * lax.axis_size("ep")
    per_group = experts // GROUPS
    args = (tokens, norm_gain, w_gate, w_up, w_down, expert_ids, combine, final_gain)
    if (
        per_group == expert_ids.shape[1] == 2
        and w_gate.shape[0] == 1
        and lax.axis_size("tp") == 2
        and GROUPS == 4
        and tokens.shape[0] % 256 == 0
    ):
        return paired(*args)
    return general(*args)


def solution(mesh):
    placed = (
        P(("grp", "ep"), "tp"),
        P("tp"),
        P("ep", None, "tp"),
        P("ep", None, "tp"),
        P("ep", "tp", None),
        P(("grp", "ep"), None),
        P(("grp", "ep"), None),
        P("tp"),
    )
    return jax.shard_map(
        body, mesh=mesh, in_specs=placed, out_specs=P(("grp", "ep"), "tp"), check_vma=False
    )
```
